256 devices in a mesh: ep: 64 (over z, y, core), tp: 4 (over x).
Axes of the slice: x: 4, y: 4, z: 8, core: 2. Of those that a mesh axis runs over, the one named last changes fastest.
Arguments:
- queries: bfloat16 [16384, 1536], P('ep', 'tp'), may hold values from -6 to 6
- kv_latent: bfloat16 [16384, 512], P('ep'), may hold values from -6 to 6
- rope_key: bfloat16 [16384, 64], P('ep'), may hold values from -6 to 6
- latent_gain: float32 [512], replicated, may hold values from 0.1 to 1.9
- w_key_up: bfloat16 [512, 1024], P(None, 'tp'), may hold values from -0.25 to 0.25
- w_value_up: bfloat16 [512, 1024], P(None, 'tp'), may hold values from -0.25 to 0.25
- query_gain: float32 [192], replicated, may hold values from 0.1 to 1.9
- key_gain: float32 [128], replicated, may hold values from 0.1 to 1.9
- rope_gain: float32 [64], replicated, may hold values from 0.1 to 1.9
- out_gain: float32 [128], replicated, may hold values from 0.1 to 1.9
- moe_tokens: bfloat16 [16384, 2048], P('ep'), may hold values from -6 to 6
- moe_gain: float32 [2048], replicated, may hold values from 0.1 to 1.9
- routes: int32 [16384, 2], P('ep'), may hold values from 0 to 63, all different within a row; in each aligned block of 64 rows (0 to 63, 64 to 127, ...) at most 3 rows name the same one
- route_weights: float32 [16384, 2], P('ep'), may hold values from 0.25 to 1
- w_gate: bfloat16 [64, 2048, 3584], P('ep', None, 'tp'), may hold values from -0.125 to 0.125
- w_up: bfloat16 [64, 2048, 3584], P('ep', None, 'tp'), may hold values from -0.125 to 0.125
- w_down: bfloat16 [64, 3584, 2048], P('ep', 'tp'), may hold values from -0.09375 to 0.09375
Outputs:
- attended: bfloat16 [16384, 1024], P('ep', 'tp')
- moe_out: bfloat16 [16384, 2048], P(('ep', 'tp'))
The draws below stay inside these ranges and needn't reach their ends.
Inputs may be any that keep to these rules, and one draw needn't show every extreme that they name: `routes`: each row names 2 different experts of 0 to 63; in each aligned block of 64 rows no expert is named by more than 3 rows, and in some block one expert is named by exactly 3.
All inputs are finite; a program needn't handle non-finite values.
Results may differ from the reference program's by a relative error of at most 0.0071.
Values may be sent and summed in bfloat16 or wider, within the bound.
No kernel may reach another device: no remote copies, remote signals or barrier semaphores. Data moves between devices by JAX's collectives and lax.ppermute only.
A program may use at most 128 MiB of HBM per device.

```python
import math
import jax
import jax.numpy as jnp
import numpy as np
from jax import lax

D = 2048
HEADS = 8
NOPE = 128
ROPE_DIM = 64
VHEAD = 128
LATENT = 512
FF = 3584
TOP = 2
EXPERTS = 64
SEQ = 16384
MOE_ROWS = 16384
Q_ROWS = 64
CAP = 3


def shard_levels(stream_key, extent, shards, least, largest):
    def one(dim, parts):
        heights = jax.random.uniform(jax.random.fold_in(jax.random.fold_in(stream_key, 6), dim), (parts,), jnp.float32, least / len(shards), largest / len(shards))
        return jnp.repeat(jnp.exp(heights), extent[dim] // parts).reshape((-1,) + (1,) * (len(extent) - dim - 1))

    level = one(*shards[0])
    for cut in shards[1:]:
        level = level * one(*cut)
    return level


def assign_block(key, own, number, rows, count, top, bound, lean):
    order = jax.random.permutation(key, count)
    heavy_load, ordinary = portions_of(count, rows * top, bound, lean, True), portions_of(count, rows * top, bound, lean, False)
    places = jnp.arange(count)

    def named(tallies, offset_by):
        used = int((tallies > 0).sum())
        fixed = max(1, used // 4)
        shifted = fixed + (places - fixed + offset_by * (used - fixed)) % max(1, count - fixed)
        return jnp.zeros((count,), jnp.int32).at[order[jnp.where(places < fixed, places, shifted)]].set(jnp.asarray(tallies, jnp.int32))

    tallies = jnp.where(number % 4 == 0, named(heavy_load, number // 4), named(ordinary, number - number // 4 - 1))
    mixed = jax.random.permutation(jax.random.fold_in(own, 3), count)
    giver, receiver = mixed[0:count // 2 * 2:2], mixed[1:count // 2 * 2:2]
    margin = jnp.minimum(tallies[giver] - 1, bound - tallies[receiver]) // 2
    margin = jnp.where((giver == order[0]) | (receiver == order[0]) | (tallies[receiver] == 0), 0, jnp.maximum(margin, 0))
    shifted = jax.random.randint(jax.random.fold_in(own, 4), (count // 2,), 0, 1 << 20) % (margin + 1)
    tallies = tallies.at[giver].add(-shifted).at[receiver].add(shifted)
    labels = jnp.searchsorted(jnp.cumsum(tallies), jnp.arange(rows * top), side="right").astype(jnp.int32)
    table = labels.reshape(top, rows).T
    table = table[jax.random.permutation(jax.random.fold_in(own, 1), rows)]
    offset_by = jax.random.randint(jax.random.fold_in(own, 2), (rows, 1), 0, top)
    return jnp.take_along_axis(table, (jnp.arange(top)[None, :] + offset_by) % top, axis=1)


def portions_of(number_of, total, most, skew, full):
    portions = [(1 << 20) // math.isqrt(standing ** skew) + 1 for standing in range(1, number_of + 1)]
    largest = most if full else min(most, max(-(-total // number_of), total * portions[0] // sum(portions)))
    least = 1 if total - largest >= number_of - 1 else 0
    given, surplus = [largest] + [least] * (number_of - 1), total - largest - least * (number_of - 1)
    while surplus > 0:
        movable = [i for i in range(1, number_of) if given[i] < largest] or [i for i in range(1, number_of) if given[i] < most]
        mass, remaining = sum([portions[i] for i in movable]), surplus
        for i in movable:
            addition = min(most - given[i], max(1, remaining * portions[i] // mass), surplus)
            given[i] = given[i] + addition
            surplus = surplus - addition
    return np.array(given)


def scatter_about(stream_key, dims, scale, limit, shards=(), held_as=jnp.bfloat16):
    drawn = scale * jax.random.normal(stream_key, dims, jnp.float32)
    if shards:
        drawn = drawn * shard_levels(stream_key, dims, shards, -0.22, 0.18)
    return jnp.clip(drawn, -limit, limit).astype(held_as)


def setup_inputs(seed: int = 0) -> dict:
    streams_of = jax.random.split(jax.random.key(seed), 18)
    queries = scatter_about(streams_of[0], (SEQ, HEADS * (NOPE + ROPE_DIM)), 1.0, 6.0, ((0, 64), (1, 4)))
    kv_latent = scatter_about(streams_of[1], (SEQ, LATENT), 1.0, 6.0, ((0, 64),))
    rope_key = scatter_about(streams_of[2], (SEQ, ROPE_DIM), 1.0, 6.0, ((0, 64),))
    latent_gain = jnp.clip(1.0 + 0.18 * jax.random.normal(streams_of[3], (LATENT,), jnp.float32), 0.1, 1.9)
    w_key_up = scatter_about(streams_of[4], (LATENT, HEADS * NOPE), LATENT ** -0.5, 0.25, ((1, 4),))
    w_value_up = scatter_about(streams_of[5], (LATENT, HEADS * VHEAD), LATENT ** -0.5, 0.25, ((1, 4),))
    query_gain = jnp.clip(1.0 + 0.18 * jax.random.normal(streams_of[6], (NOPE + ROPE_DIM,), jnp.float32), 0.1, 1.9)
    key_gain = jnp.clip(1.0 + 0.18 * jax.random.normal(streams_of[7], (NOPE,), jnp.float32), 0.1, 1.9)
    rope_gain = jnp.clip(1.0 + 0.18 * jax.random.normal(streams_of[8], (ROPE_DIM,), jnp.float32), 0.1, 1.9)
    out_gain = jnp.clip(1.0 + 0.18 * jax.random.normal(streams_of[9], (VHEAD,), jnp.float32), 0.1, 1.9)
    moe_tokens = scatter_about(streams_of[10], (MOE_ROWS, D), 1.0, 6.0, ((0, 64),))
    moe_gain = jnp.clip(1.0 + 0.18 * jax.random.normal(streams_of[11], (D,), jnp.float32), 0.1, 1.9)
    routes_keys = jax.random.split(jax.random.fold_in(streams_of[12], 1), MOE_ROWS // Q_ROWS)
    routes_turns = jax.random.permutation(jax.random.fold_in(streams_of[12], 3), MOE_ROWS // Q_ROWS)
    routes = jax.vmap(lambda own, number: assign_block(jax.random.fold_in(streams_of[12], 2), own, number, Q_ROWS, EXPERTS, TOP, CAP, 1))(routes_keys, routes_turns).reshape((MOE_ROWS, TOP))
    route_weights = jnp.clip(0.25 + 0.75 * jax.random.uniform(streams_of[13], (MOE_ROWS, TOP), jnp.float32) ** shard_levels(streams_of[13], (MOE_ROWS, TOP), ((0, 64),), -0.2, 0.2), 0.25, 1.0)
    w_gate = scatter_about(streams_of[14], (EXPERTS, D, FF), D ** -0.5, 0.125, ((0, 64), (2, 4)))
    w_up = scatter_about(streams_of[15], (EXPERTS, D, FF), D ** -0.5, 0.125, ((0, 64), (2, 4)))
    w_down = scatter_about(streams_of[16], (EXPERTS, FF, D), FF ** -0.5, 0.09375, ((0, 64), (1, 4)))
    return {"queries": queries, "kv_latent": kv_latent, "rope_key": rope_key, "latent_gain": latent_gain, "w_key_up": w_key_up, "w_value_up": w_value_up, "query_gain": query_gain, "key_gain": key_gain, "rope_gain": rope_gain, "out_gain": out_gain, "moe_tokens": moe_tokens, "moe_gain": moe_gain, "routes": routes, "route_weights": route_weights, "w_gate": w_gate, "w_up": w_up, "w_down": w_down}


EPS = 1e-06
THETA = 500000.0

def rms_norm(values, norm_gain):
    return values * lax.rsqrt(lax.optimization_barrier(jnp.mean(values * values, axis=-1, keepdims=True)) + EPS) * norm_gain

def rounded(values):
    return lax.optimization_barrier(values.astype(jnp.bfloat16))

def rope_tables(positions, rope_dim):
    freqs = 1.0 / THETA ** (jnp.arange(0, rope_dim, 2, dtype=jnp.float32) / rope_dim)
    angles = positions.astype(jnp.float32)[:, None] * freqs[None, :]
    return (jnp.cos(angles), jnp.sin(angles))

def rotate(values, rot_cos, rot_sin):
    half_dim = values.shape[-1] // 2
    first_half = values[..., :half_dim]
    second_half = values[..., half_dim:]
    return jnp.concatenate([first_half * rot_cos - second_half * rot_sin, second_half * rot_cos + first_half * rot_sin], axis=-1)

def attention(queries, kv_latent, rope_key, latent_gain, w_key_up, w_value_up, query_gain, key_gain, rope_gain, out_gain):
    seq_len = queries.shape[0]
    positions = jnp.arange(seq_len, dtype=jnp.int32)
    rot_cos, rot_sin = rope_tables(positions, ROPE_DIM)
    latent = rounded(rms_norm(kv_latent.astype(jnp.float32), latent_gain))
    key_nope = jnp.dot(latent, w_key_up, preferred_element_type=jnp.float32).reshape(seq_len, HEADS, NOPE)
    key_nope = rounded(rms_norm(key_nope, key_gain)).astype(jnp.float32)
    values = rounded(jnp.dot(latent, w_value_up, preferred_element_type=jnp.float32))
    values = values.astype(jnp.float32).reshape(seq_len, HEADS, VHEAD)
    rot_key = rounded(rotate(rms_norm(rope_key.astype(jnp.float32), rope_gain), rot_cos, rot_sin)).astype(jnp.float32)
    query = rms_norm(queries.astype(jnp.float32).reshape(seq_len, HEADS, NOPE + ROPE_DIM), query_gain)
    query_nope = rounded(query[..., :NOPE]).astype(jnp.float32)
    query_rope = rounded(rotate(query[..., NOPE:], rot_cos[:, None, :], rot_sin[:, None, :])).astype(jnp.float32)
    scale = (NOPE + ROPE_DIM) ** (-0.5)
    block_rows = math.gcd(seq_len, 512)

    def one_block(block_index):
        block_first = block_index * block_rows
        q_nope = lax.dynamic_slice_in_dim(query_nope, block_first, block_rows, 0)
        q_rope = lax.dynamic_slice_in_dim(query_rope, block_first, block_rows, 0)
        scores = (jnp.einsum('qhd,khd->hqk', q_nope, key_nope, precision=lax.Precision.HIGHEST) + jnp.einsum('qhr,kr->hqk', q_rope, rot_key, precision=lax.Precision.HIGHEST)) * scale
        query_pos = block_first + jnp.arange(block_rows, dtype=jnp.int32)
        visible = (query_pos[:, None] >= positions[None, :])[None]
        exp_scores = jnp.where(visible, jnp.exp(scores), 0.0)
        denominator = lax.optimization_barrier(jnp.sum(exp_scores, axis=-1))
        weighted = jnp.einsum('hqk,khd->qhd', rounded(exp_scores).astype(jnp.float32), values, precision=lax.Precision.HIGHEST)
        mixed = weighted / jnp.transpose(denominator)[:, :, None]
        return rms_norm(mixed, out_gain).astype(jnp.bfloat16).reshape(block_rows, HEADS * VHEAD)
    blocks = lax.map(one_block, jnp.arange(seq_len // block_rows, dtype=jnp.int32))
    return blocks.reshape(seq_len, HEADS * VHEAD)

def experts_layer(moe_tokens, moe_gain, routes, route_weights, w_gate, w_up, w_down):
    n_rows = moe_tokens.shape[0]
    normed = rounded(rms_norm(moe_tokens.astype(jnp.float32), moe_gain))
    n_blocks = n_rows // Q_ROWS
    assigned = Q_ROWS * TOP
    slot_count = EXPERTS * CAP
    chosen = routes.reshape(n_blocks, assigned)
    onehot = (chosen[..., None] == jnp.arange(EXPERTS, dtype=jnp.int32)).astype(jnp.int32)
    rank = lax.optimization_barrier(jnp.sum((jnp.cumsum(onehot, axis=1) - onehot) * onehot, axis=-1)).astype(jnp.int32)
    slots = chosen * CAP + rank
    row_ids = jnp.arange(n_blocks, dtype=jnp.int32)[:, None] * Q_ROWS + jnp.arange(assigned, dtype=jnp.int32)[None, :] // TOP
    slot_hit = (slots[..., None] == jnp.arange(slot_count, dtype=jnp.int32)).astype(jnp.int32)
    table = lax.optimization_barrier(jnp.sum(slot_hit * (row_ids[..., None] + 1), axis=1)) - 1
    table = jnp.where(table < 0, n_rows, table).astype(jnp.int32)
    padded = jnp.concatenate([normed, jnp.zeros((1, normed.shape[1]), jnp.bfloat16)], axis=0)

    def one_expert(expert):
        rows_used = lax.dynamic_slice_in_dim(table, expert * CAP, CAP, 1).reshape(-1)
        inputs = padded[rows_used]
        gate = jnp.dot(inputs, w_gate[expert], preferred_element_type=jnp.float32)
        upward = jnp.dot(inputs, w_up[expert], preferred_element_type=jnp.float32)
        hidden = (jax.nn.silu(gate) * upward).astype(jnp.bfloat16)
        return rounded(jnp.dot(hidden, w_down[expert], preferred_element_type=jnp.float32))
    outputs = lax.map(one_expert, jnp.arange(EXPERTS, dtype=jnp.int32))
    place = jnp.arange(n_blocks, dtype=jnp.int32)[:, None] * CAP + rank
    picked = outputs[chosen, place].astype(jnp.float32)
    scaled = picked * route_weights.reshape(n_blocks, assigned)[..., None]
    mixed = lax.optimization_barrier(jnp.sum(scaled.reshape(n_rows, TOP, picked.shape[-1]), axis=1))
    return mixed.astype(jnp.bfloat16)

def reference(queries, kv_latent, rope_key, latent_gain, w_key_up, w_value_up, query_gain, key_gain, rope_gain, out_gain, moe_tokens, moe_gain, routes, route_weights, w_gate, w_up, w_down):
    attended = attention(queries, kv_latent, rope_key, latent_gain, w_key_up, w_value_up, query_gain, key_gain, rope_gain, out_gain)
    moe_out = experts_layer(moe_tokens, moe_gain, routes, route_weights, w_gate, w_up, w_down)
    return (attended, moe_out)
```

```python
import functools

import jax
import jax.numpy as jnp
from jax import lax
from jax.experimental import pallas as pl
from jax.experimental.pallas import tpu as pltpu
from jax.sharding import Mesh
from jax.sharding import PartitionSpec as P

ZY = ("ep_0", "ep_1")
CORE = "ep_2"
EP = ("ep_0", "ep_1", "ep_2")
EP_TP = ("ep_0", "ep_1", "ep_2", "tp")

EPS = 1e-06
THETA = 500000.0
LOG2E = 1.4426950408889634


def rms_norm(values, norm_gain):
    return values * lax.rsqrt(jnp.mean(values * values, axis=-1, keepdims=True) + EPS) * norm_gain


def rope_tables(positions, rope_dim):
    freqs = 1.0 / THETA ** (jnp.arange(0, rope_dim, 2, dtype=jnp.float32) / rope_dim)
    angles = positions.astype(jnp.float32)[:, None] * freqs[None, :]
    return (jnp.cos(angles), jnp.sin(angles))


def rotate(values, rot_cos, rot_sin):
    half_dim = values.shape[-1] // 2
    first_half = values[..., :half_dim]
    second_half = values[..., half_dim:]
    return jnp.concatenate(
        [
            first_half * rot_cos - second_half * rot_sin,
            second_half * rot_cos + first_half * rot_sin,
        ],
        axis=-1,
    )


def flash_body(block_rows, chunk_blocks, rows_per_block, scale, idx_ref, q_ref, kv_ref, gain_ref, out_ref, acc_ref):
    step = pl.program_id(0)
    idx = idx_ref[0]
    heads = q_ref.shape[0]
    half = block_rows // 2
    rope_lanes = 64

    @pl.when(step == 0)
    def _():
        acc_ref[...] = jnp.zeros_like(acc_ref)

    ones = jnp.ones((block_rows, 128), jnp.bfloat16)

    def block(local, masked):
        base = local * rows_per_block
        rope = kv_ref[pl.ds(base + 4 * block_rows, half), :]
        rope_rolled = pltpu.roll(rope.astype(jnp.float32), rope_lanes, 1).astype(jnp.bfloat16)
        rope_all = jnp.concatenate([rope, rope_rolled], axis=0)
        for h in range(heads):
            keys = kv_ref[pl.ds(base + h * block_rows, block_rows), :]
            vals = kv_ref[pl.ds(base + (heads + h) * block_rows, block_rows), :]
            key_tile = jnp.concatenate([keys, rope_all], axis=1)
            scores = lax.dot_general(
                q_ref[h], key_tile, (((1,), (1,)), ((), ())), preferred_element_type=jnp.float32
            )
            soft = jnp.exp2(scores * (scale * LOG2E))
            if masked:
                qi = lax.broadcasted_iota(jnp.int32, soft.shape, 0)
                ki = lax.broadcasted_iota(jnp.int32, soft.shape, 1)
                soft = jnp.where(qi >= ki, soft, 0.0)
            val_tile = jnp.concatenate([vals, ones], axis=1)
            acc_ref[h] += jnp.dot(
                soft.astype(jnp.bfloat16), val_tile, preferred_element_type=jnp.float32
            )

    first = step * chunk_blocks
    for local in range(chunk_blocks):

        @pl.when(first + local < idx)
        def _():
            block(local, False)

        @pl.when(first + local == idx)
        def _():
            block(local, True)

    @pl.when(step == pl.num_programs(0) - 1)
    def _():
        for h in range(heads):
            acc = acc_ref[h]
            mixed = acc[:, :128] / acc[:, 128:]
            out = rms_norm(mixed, gain_ref[...])
            out_ref[:, h * 128 : (h + 1) * 128] = out.astype(jnp.bfloat16)


def flash(idx, q_full, gathered, out_gain, blocks, scale):
    heads, block_rows, _ = q_full.shape
    rows_per_block = gathered.shape[0] // blocks
    chunk_blocks = 4
    chunk_rows = chunk_blocks * rows_per_block
    steps = blocks // chunk_blocks
    grid_spec = pltpu.PrefetchScalarGridSpec(
        num_scalar_prefetch=1,
        grid=(steps,),
        in_specs=[
            pl.BlockSpec(q_full.shape, lambda s, i: (0, 0, 0)),
            pl.BlockSpec((chunk_rows, 128), lambda s, i: (jnp.minimum(s, i[0] // chunk_blocks), 0)),
            pl.BlockSpec((1, 128), lambda s, i: (0, 0)),
        ],
        out_specs=pl.BlockSpec((block_rows, heads * 128), lambda s, i: (0, 0)),
        scratch_shapes=[pltpu.VMEM((heads, block_rows, 256), jnp.float32)],
    )
    flops = 2 * heads * block_rows * block_rows * blocks * 512
    return pl.pallas_call(
        functools.partial(flash_body, block_rows, chunk_blocks, rows_per_block, scale),
        grid_spec=grid_spec,
        out_shape=jax.ShapeDtypeStruct((block_rows, heads * 128), jnp.bfloat16),
        cost_estimate=pl.CostEstimate(
            flops=flops, bytes_accessed=gathered.size * 2, transcendentals=heads * block_rows * block_rows * blocks
        ),
        compiler_params=pltpu.CompilerParams(dimension_semantics=("arbitrary",), vmem_limit_bytes=40 << 20),
        name="flash",
    )(idx, q_full, gathered, out_gain)


def attention_send(kv_latent, rope_key, latent_gain, w_key_up, w_value_up, key_gain, rope_gain, rot):
    tok_rows = kv_latent.shape[0]
    nope_dim = key_gain.shape[0]
    head_count = w_key_up.shape[1] // nope_dim
    rot_cos, rot_sin = rot
    latent = rms_norm(kv_latent.astype(jnp.float32), latent_gain).astype(jnp.bfloat16)
    key_nope = jnp.dot(latent, w_key_up, preferred_element_type=jnp.float32)
    values = jnp.dot(latent, w_value_up, preferred_element_type=jnp.float32).astype(jnp.bfloat16)
    rot_key = rotate(rms_norm(rope_key.astype(jnp.float32), rope_gain), rot_cos, rot_sin).astype(jnp.bfloat16)
    pieces = []
    for h in range(head_count):
        piece = key_nope[:, h * nope_dim : (h + 1) * nope_dim]
        pieces.append(rms_norm(piece, key_gain).astype(jnp.bfloat16))
    for h in range(head_count):
        pieces.append(values[:, h * 128 : (h + 1) * 128])
    half = tok_rows // 2
    pieces.append(jnp.concatenate([rot_key[:half], rot_key[half:]], axis=1))
    return jnp.concatenate(pieces, axis=0)


def attention_queries(queries, query_gain, nope_dim, rot):
    tok_rows = queries.shape[0]
    q_dim = query_gain.shape[0]
    head_count = queries.shape[1] // q_dim
    rot_cos, rot_sin = rot
    heads = []
    for h in range(head_count):
        query = rms_norm(queries[:, h * q_dim : (h + 1) * q_dim].astype(jnp.float32), query_gain)
        roped = rotate(query[:, nope_dim:], rot_cos, rot_sin)
        pad = jnp.zeros((tok_rows, 256 - q_dim), jnp.float32)
        heads.append(jnp.concatenate([query[:, :nope_dim], roped, pad], axis=1).astype(jnp.bfloat16))
    return jnp.stack(heads)


def mlp_body(k_steps, *refs):
    x_refs = refs[:4]
    wg_ref, wu_ref, wd_ref = refs[4:7]
    out_refs = refs[7:11]
    gate_ref, up_ref, hid_ref = refs[11:14]
    step = pl.program_id(0)
    k_rows = wg_ref.shape[0]
    rows = x_refs[0].shape[0]

    @pl.when(step < k_steps)
    def _():
        cols = pl.ds(pl.multiple_of(jnp.minimum(step, k_steps - 1) * k_rows, k_rows), k_rows)
        x = jnp.concatenate([r[:, cols] for r in x_refs], axis=0)
        gate = jnp.dot(x, wg_ref[...], preferred_element_type=jnp.float32)
        up = jnp.dot(x, wu_ref[...], preferred_element_type=jnp.float32)

        @pl.when(step == 0)
        def _():
            gate_ref[...] = gate
            up_ref[...] = up

        @pl.when(step > 0)
        def _():
            gate_ref[...] += gate
            up_ref[...] += up

    @pl.when(step == k_steps)
    def _():
        gate = gate_ref[...]
        hid_ref[...] = (gate / (1.0 + jnp.exp(-gate)) * up_ref[...]).astype(jnp.bfloat16)

    @pl.when(step >= k_steps)
    def _():
        y = jnp.dot(hid_ref[...], wd_ref[...], preferred_element_type=jnp.float32)
        for k, ref in enumerate(out_refs):
            ref[...] = y[k * rows : (k + 1) * rows].astype(ref.dtype)


def mlp(xs, w_gate, w_up, w_down):
    rows, dim = xs[0].shape
    hid = w_gate.shape[1]
    k_steps = 4
    n_steps = 4
    kb = dim // k_steps
    nb = dim // n_steps

    def w_in(s):
        return (jnp.minimum(s, k_steps - 1), 0)

    def w_out(s):
        return (0, jnp.maximum(s - k_steps, 0))

    dtypes = [jnp.float32, jnp.bfloat16, jnp.bfloat16, jnp.bfloat16]
    return pl.pallas_call(
        functools.partial(mlp_body, k_steps),
        grid=(k_steps + n_steps,),
        in_specs=[pl.BlockSpec((rows, dim), lambda s: (0, 0))] * 4
        + [
            pl.BlockSpec((kb, hid), w_in),
            pl.BlockSpec((kb, hid), w_in),
            pl.BlockSpec((hid, nb), w_out),
        ],
        out_specs=[pl.BlockSpec((rows, nb), w_out)] * 4,
        out_shape=[jax.ShapeDtypeStruct((rows, dim), d) for d in dtypes],
        scratch_shapes=[
            pltpu.VMEM((4 * rows, hid), jnp.float32),
            pltpu.VMEM((4 * rows, hid), jnp.float32),
            pltpu.VMEM((4 * rows, hid), jnp.bfloat16),
        ],
        cost_estimate=pl.CostEstimate(
            flops=2 * 4 * rows * dim * hid * 3, bytes_accessed=3 * dim * hid * 2, transcendentals=4 * rows * hid
        ),
        compiler_params=pltpu.CompilerParams(dimension_semantics=("arbitrary",), vmem_limit_bytes=48 << 20),
        name="mlp",
    )(*xs, w_gate, w_up, w_down)


def shifted(x, axis, by):
    count = lax.axis_size(axis)
    return lax.ppermute(x, axis, [(i, (i + by) % count) for i in range(count)])


def routing(routes, experts, capacity, zy_count):
    part_rows, top_count = routes.shape
    chosen = routes.reshape(part_rows * top_count)
    order = jnp.arange(part_rows * top_count, dtype=jnp.int32)
    earlier = (chosen[:, None] == chosen[None, :]) & (order[None, :] < order[:, None])
    rank = jnp.sum(earlier.astype(jnp.int32), axis=1)
    away = (chosen % 2) ^ lax.axis_index(CORE)
    slots = away * (zy_count * capacity) + (chosen // 2) * capacity + rank
    slot_ids = jnp.arange(experts * capacity, dtype=jnp.int32)
    hit = (slots[:, None] == slot_ids[None, :]).astype(jnp.bfloat16)
    return hit.reshape(part_rows, top_count, experts * capacity)


def experts_part(moe_tokens, moe_gain, routes, route_weights, w_gate, w_up, w_down):
    n_rows = moe_tokens.shape[0]
    top_count = routes.shape[1]
    quarters = lax.axis_size("tp")
    part_rows = n_rows // quarters
    experts = lax.axis_size(EP)
    zy_count = lax.axis_size(ZY)
    capacity = (3 * top_count * part_rows + 2 * experts - 1) // (2 * experts)
    my_part = lax.axis_index("tp")
    first = my_part * part_rows
    own_rows = lax.dynamic_slice_in_dim(moe_tokens, first, part_rows, 0)
    normed = rms_norm(own_rows.astype(jnp.float32), moe_gain).astype(jnp.bfloat16)
    own_routes = lax.dynamic_slice_in_dim(routes, first, part_rows, 0)
    own_weights = lax.dynamic_slice_in_dim(route_weights, first, part_rows, 0)
    hit = routing(own_routes, experts, capacity, zy_count)
    send = jnp.sum(hit, axis=1)
    half = zy_count * capacity

    def outgoing(cols):
        return jnp.einsum("rs,rd->sd", cols, normed, preferred_element_type=jnp.float32).astype(jnp.bfloat16)

    near = outgoing(send[:, :half])
    far = shifted(outgoing(send[:, half:]), CORE, 1)

    def dispatch(rows):
        return lax.all_to_all(rows, ZY, 0, 0, tiled=True)

    def spread(rows):
        return [rows, shifted(rows, "tp", 1), shifted(rows, "tp", -1), shifted(rows, "tp", 2)]

    def total(parts):
        back = [parts[0], shifted(parts[1], "tp", -1), shifted(parts[2], "tp", 1), shifted(parts[3], "tp", 2)]
        whole = back[0]
        for part in back[1:]:
            whole = whole + part.astype(jnp.float32)
        return whole.astype(jnp.bfloat16)

    near_x = spread(dispatch(near))
    far_x = spread(dispatch(far))
    near_y = mlp(near_x, w_gate[0], w_up[0], w_down[0])
    far_y = mlp(far_x, w_gate[0], w_up[0], w_down[0])
    near_back = dispatch(total(near_y))
    far_back = shifted(dispatch(total(far_y)), CORE, 1)
    picked = jnp.einsum("rks,sd->rkd", hit[..., :half], near_back, preferred_element_type=jnp.float32) + jnp.einsum(
        "rks,sd->rkd", hit[..., half:], far_back, preferred_element_type=jnp.float32
    )
    return jnp.sum(picked * own_weights[:, :, None], axis=1).astype(jnp.bfloat16)


def on_device(
    queries,
    kv_latent,
    rope_key,
    latent_gain,
    w_key_up,
    w_value_up,
    query_gain,
    key_gain,
    rope_gain,
    out_gain,
    moe_tokens,
    moe_gain,
    routes,
    route_weights,
    w_gate,
    w_up,
    w_down,
):
    tok_rows = queries.shape[0]
    index = lax.axis_index(EP)
    positions = index * tok_rows + jnp.arange(tok_rows, dtype=jnp.int32)
    rot = rope_tables(positions, rope_key.shape[1])
    sent = attention_send(kv_latent, rope_key, latent_gain, w_key_up, w_value_up, key_gain, rope_gain, rot)
    gathered = lax.all_gather(sent, EP, axis=0, tiled=True)
    q_full = attention_queries(queries, query_gain, key_gain.shape[0], rot)
    moe_out = experts_part(moe_tokens, moe_gain, routes, route_weights, w_gate, w_up, w_down)
    attended = flash(
        index.reshape(1).astype(jnp.int32),
        q_full,
        gathered,
        out_gain.reshape(1, -1),
        lax.axis_size(EP),
        query_gain.shape[0] ** -0.5,
    )
    return (attended, moe_out)


def solution(mesh):
    finer = Mesh(mesh.devices.reshape(8, 4, 2, mesh.shape["tp"]), ("ep_0", "ep_1", "ep_2", "tp"))
    placed = (
        P(EP, "tp"),
        P(EP, None),
        P(EP, None),
        P(),
        P(None, "tp"),
        P(None, "tp"),
        P(),
        P(),
        P(),
        P(),
        P(EP, None),
        P(),
        P(EP, None),
        P(EP, None),
        P(EP, None, "tp"),
        P(EP, None, "tp"),
        P(EP, "tp", None),
    )
    return jax.shard_map(
        on_device,
        mesh=finer,
        in_specs=placed,
        out_specs=(P(EP, "tp"), P(EP_TP, None)),
        check_vma=False,
    )
```

```python
import functools

import jax
import jax.numpy as jnp
from jax import lax
from jax.experimental import pallas as pl
from jax.experimental.pallas import tpu as pltpu
from jax.sharding import Mesh
from jax.sharding import PartitionSpec as P

ZY = ("ep_0", "ep_1")
CORE = "ep_2"
YC = ("ep_1", "ep_2")
EP = ("ep_0", "ep_1", "ep_2")
EP_TP = ("ep_0", "ep_1", "ep_2", "tp")

EPS = 1e-06
THETA = 500000.0
LOG2E = 1.4426950408889634


def rms_norm(values, norm_gain):
    return values * lax.rsqrt(jnp.mean(values * values, axis=-1, keepdims=True) + EPS) * norm_gain


def in_hbm(x):
    return pltpu.with_memory_space_constraint(x, pltpu.HBM)


def swap_halves(v):
    lane = lax.broadcasted_iota(jnp.int32, v.shape, 1)
    return jnp.where(lane % 64 < 32, pltpu.roll(v, 96, 1), pltpu.roll(v, 32, 1))


def prepare_body(*refs):
    sources = refs[:11]
    keys_out, queries_out = refs[11:13]
    queries_ref, latent_ref, rope_ref, latent_gain, wk_ref, wv_ref, query_gain, key_gain, rope_gain, cos_ref, sin_ref = (
        refs[13:24]
    )
    sem = refs[24]
    copies = [pltpu.make_async_copy(s, d, sem.at[k]) for k, (s, d) in enumerate(zip(sources, refs[13:24]))]
    for copy in copies:
        copy.start()
    for copy in copies:
        copy.wait()
    rows = latent_ref.shape[0]
    half = rows // 2
    heads = wk_ref.shape[1] // 128
    latent = rms_norm(latent_ref[...].astype(jnp.float32), latent_gain[...]).astype(jnp.bfloat16)
    keys = jnp.dot(latent, wk_ref[...], preferred_element_type=jnp.float32)
    values = jnp.dot(latent, wv_ref[...], preferred_element_type=jnp.float32)
    for h in range(heads):
        cols = slice(h * 128, (h + 1) * 128)
        keys_out[h * rows : (h + 1) * rows, :] = rms_norm(keys[:, cols], key_gain[...]).astype(jnp.bfloat16)
        keys_out[(heads + h) * rows : (heads + h + 1) * rows, :] = values[:, cols].astype(jnp.bfloat16)
    cos = cos_ref[...]
    sin = sin_ref[...]
    lane = lax.broadcasted_iota(jnp.int32, (half, 128), 1)
    rope = rms_norm(rope_ref[...].astype(jnp.float32), rope_gain[...])
    rope = jnp.concatenate([rope[:half], rope[half:]], axis=1)
    cos_k = jnp.where(lane < 64, cos[:half], cos[half:])
    sin_k = jnp.where(lane < 64, sin[:half], sin[half:])
    keys_out[2 * heads * rows :, :] = (rope * cos_k + swap_halves(rope) * sin_k).astype(jnp.bfloat16)
    ropes = []
    for h in range(heads):
        query = rms_norm(queries_ref[:, h * 192 : (h + 1) * 192].astype(jnp.float32), query_gain[...])
        queries_out[h * rows : (h + 1) * rows, :] = query[:, :128].astype(jnp.bfloat16)
        ropes.append(query[:, 128:])
    rope = jnp.concatenate(ropes, axis=1)
    queries_out[heads * rows :, :] = (rope * cos + swap_halves(rope) * sin).astype(jnp.bfloat16)


def prepare(queries, kv_latent, rope_key, latent_gain, w_key_up, w_value_up, query_gain, key_gain, rope_gain, positions):
    rows = queries.shape[0]
    rope_dim = rope_key.shape[1]
    freqs = 1.0 / THETA ** (jnp.arange(0, rope_dim, 2, dtype=jnp.float32) / rope_dim)
    lane = jnp.arange(128, dtype=jnp.int32)
    angles = positions.astype(jnp.float32)[:, None] * jnp.tile(freqs, 4)[None, :]
    sign = jnp.where(lane % 64 < 32, -1.0, 1.0)[None, :]
    args = (
        queries, kv_latent, rope_key, latent_gain.reshape(1, -1), w_key_up, w_value_up, query_gain.reshape(1, -1),
        key_gain.reshape(1, -1), rope_gain.reshape(1, -1), jnp.cos(angles), jnp.sin(angles) * sign,
    )
    return pl.pallas_call(
        prepare_body,
        in_specs=[pl.BlockSpec(memory_space=pltpu.HBM)] * len(args),
        out_specs=[pl.BlockSpec(memory_space=pltpu.VMEM)] * 2,
        scratch_shapes=[pltpu.VMEM(a.shape, a.dtype) for a in args] + [pltpu.SemaphoreType.DMA((len(args),))],
        out_shape=[
            jax.ShapeDtypeStruct((rows * 9 // 2, 128), jnp.bfloat16),
            jax.ShapeDtypeStruct((rows * 3, 128), jnp.bfloat16),
        ],
        cost_estimate=pl.CostEstimate(flops=rows * 512 * 512 * 2, bytes_accessed=2 << 20, transcendentals=0),
        compiler_params=pltpu.CompilerParams(vmem_limit_bytes=16 << 20),
        name="prepare",
    )(*[in_hbm(a) for a in args])


def flash_body(groups, rows, scale, at_ref, q_hbm, kv_hbm, out_ref, kt_ref, vt_ref, all_q_ref, kv_ref, sem):
    tile = pl.program_id(0)
    group = at_ref[0]
    place = at_ref[1]
    heads = 2
    half = rows // 2
    per = kv_ref.shape[0] // groups

    @pl.when(tile == 0)
    def _():
        lane = lax.broadcasted_iota(jnp.int32, (rows, 128), 1)
        copies = []
        for g in range(groups):
            part = pl.ds(g * per, per)
            copies.append(pltpu.make_async_copy(kv_hbm.at[part], kv_ref.at[part], sem.at[g]))
        copies.append(pltpu.make_async_copy(q_hbm, all_q_ref, sem.at[groups]))
        for copy in copies:
            copy.start()
        for g in range(groups):
            copies[g].wait()
            base = g * per
            seen = jnp.where(g <= group, 1.0, 0.0).astype(jnp.float32)
            rope = kv_ref[base + 2 * heads * rows : base + per, :].astype(jnp.float32)
            turned = pltpu.roll(rope, 64, 1)
            low = jnp.where(lane < 64, jnp.concatenate([rope, turned], axis=0), 0.0).astype(jnp.bfloat16)
            high = jnp.where(lane >= 64, jnp.concatenate([turned, rope], axis=0), 0.0).astype(jnp.bfloat16)
            for h in range(heads):
                kt_ref[g * heads + h, :, :128] = kv_ref[base + h * rows : base + (h + 1) * rows, :]
                kt_ref[g * heads + h, :, 128:] = low if h == 0 else high
                vals = kv_ref[base + (heads + h) * rows : base + (heads + h + 1) * rows, :].astype(jnp.float32)
                vt_ref[g * heads + h, :, :128] = (vals * seen).astype(jnp.bfloat16)
                vt_ref[g * heads + h, :, 128:] = jnp.full((rows, 128), seen, jnp.float32).astype(jnp.bfloat16)

        copies[groups].wait()

    q_ref = all_q_ref.at[pl.ds(pl.multiple_of(tile * 3 * rows, 3 * rows), 3 * rows)]
    q_rope = q_ref[heads * rows :, :]
    sums = []
    for h in range(heads):
        query = jnp.concatenate([q_ref[h * rows : (h + 1) * rows, :], q_rope], axis=1)
        total = None
        for k in range(groups):
            at = ((group + k) % groups) * heads + h
            scores = lax.dot_general(
                query, kt_ref[at], (((1,), (1,)), ((), ())), preferred_element_type=jnp.float32
            )
            soft = jnp.exp2(scores * (scale * LOG2E))
            if k == 0:
                qi = lax.broadcasted_iota(jnp.int32, soft.shape, 0) + (tile - place) * rows
                ki = lax.broadcasted_iota(jnp.int32, soft.shape, 1)
                soft = jnp.where(qi >= ki, soft, 0.0)
            part = jnp.dot(soft.astype(jnp.bfloat16), vt_ref[at], preferred_element_type=jnp.float32)
            total = part if total is None else total + part
        out_ref[h * rows : (h + 1) * rows, :] = total[:, :128].astype(jnp.bfloat16)
        for t in range(2):
            den = total[t * half : (t + 1) * half, 128:]
            ri = lax.broadcasted_iota(jnp.int32, den.shape, 0)
            ci = lax.broadcasted_iota(jnp.int32, den.shape, 1)
            sums.append(jnp.sum(jnp.where(ri == ci, den, 0.0), axis=0, keepdims=True))
    sums = jnp.concatenate(sums + [jnp.zeros((4, 128), jnp.float32)], axis=0)
    high = sums.astype(jnp.bfloat16).astype(jnp.float32)
    low = sums - high
    out_ref[heads * rows :, :] = jnp.concatenate([high, low], axis=0).astype(jnp.bfloat16)


def flash(at, queries, keys, groups, scale):
    rows = keys.shape[0] // groups * 2 // 9
    tiles = queries.shape[0] // (3 * rows)
    out_rows = 2 * rows + 16
    grid_spec = pltpu.PrefetchScalarGridSpec(
        num_scalar_prefetch=1,
        grid=(tiles,),
        in_specs=[
            pl.BlockSpec(memory_space=pltpu.HBM),
            pl.BlockSpec(memory_space=pltpu.HBM),
        ],
        out_specs=pl.BlockSpec((out_rows, 128), lambda s, i: (s, 0)),
        scratch_shapes=[
            pltpu.VMEM((2 * groups, rows, 256), jnp.bfloat16),
            pltpu.VMEM((2 * groups, rows, 256), jnp.bfloat16),
            pltpu.VMEM(queries.shape, jnp.bfloat16),
            pltpu.VMEM(keys.shape, jnp.bfloat16),
            pltpu.SemaphoreType.DMA((groups + 1,)),
        ],
    )
    pairs = 2 * rows * rows * groups * tiles
    return pl.pallas_call(
        functools.partial(flash_body, groups, rows, scale),
        grid_spec=grid_spec,
        out_shape=jax.ShapeDtypeStruct((tiles * out_rows, 128), jnp.bfloat16),
        cost_estimate=pl.CostEstimate(flops=pairs * 1024, bytes_accessed=4 << 20, transcendentals=pairs),
        compiler_params=pltpu.CompilerParams(dimension_semantics=("arbitrary",), vmem_limit_bytes=24 << 20),
        name="flash",
    )(at, in_hbm(queries), in_hbm(keys))


def finish_body(count, in_ref, gain_ref, out_ref):
    per = in_ref.shape[0] // count
    rows = out_ref.shape[0]
    half = rows // 2
    total = in_ref[:per, :].astype(jnp.float32)
    for k in range(1, count):
        total = total + in_ref[k * per : (k + 1) * per, :].astype(jnp.float32)
    sums = total[2 * rows : 2 * rows + 8] + total[2 * rows + 8 : 2 * rows + 16]
    ri = lax.broadcasted_iota(jnp.int32, (half, 128), 0)
    ci = lax.broadcasted_iota(jnp.int32, (half, 128), 1)
    for h in range(2):
        for t in range(2):
            den = jnp.sum(jnp.where(ri == ci, sums[2 * h + t : 2 * h + t + 1], 0.0), axis=1, keepdims=True)
            mixed = total[h * rows + t * half : h * rows + (t + 1) * half] / den
            out_ref[t * half : (t + 1) * half, h * 128 : (h + 1) * 128] = rms_norm(mixed, gain_ref[...]).astype(
                jnp.bfloat16
            )


def finish(parts, out_gain, count, rows):
    whole = pl.BlockSpec(memory_space=pltpu.VMEM)
    return pl.pallas_call(
        functools.partial(finish_body, count),
        in_specs=[whole, whole],
        out_specs=whole,
        out_shape=jax.ShapeDtypeStruct((rows, 256), jnp.bfloat16),
        compiler_params=pltpu.CompilerParams(vmem_limit_bytes=16 << 20),
        name="finish",
    )(parts, out_gain.reshape(1, -1))


def mlp_body(*refs):
    x_refs = refs[:4]
    wg_ref, wu_ref, wd_ref = refs[4:7]
    out_refs = refs[7:11]
    rows = x_refs[0].shape[0]
    x = jnp.concatenate([r[...] for r in x_refs], axis=0)
    gate = jnp.dot(x, wg_ref[...], preferred_element_type=jnp.float32)
    up = jnp.dot(x, wu_ref[...], preferred_element_type=jnp.float32)
    hidden = (gate / (1.0 + jnp.exp(-gate)) * up).astype(jnp.bfloat16)
    y = jnp.dot(hidden, wd_ref[...], preferred_element_type=jnp.float32)
    for k, ref in enumerate(out_refs):
        ref[...] = y[k * rows : (k + 1) * rows].astype(ref.dtype)


def mlp(xs, w_gate, w_up, w_down):
    rows, dim = xs[0].shape
    hid = w_gate.shape[1]
    whole = pl.BlockSpec(memory_space=pltpu.VMEM)
    dtypes = [jnp.float32, jnp.bfloat16, jnp.bfloat16, jnp.bfloat16]
    return pl.pallas_call(
        mlp_body,
        in_specs=[whole] * 7,
        out_specs=[whole] * 4,
        out_shape=[jax.ShapeDtypeStruct((rows, dim), d) for d in dtypes],
        cost_estimate=pl.CostEstimate(
            flops=2 * 4 * rows * dim * hid * 3, bytes_accessed=3 * dim * hid * 2, transcendentals=4 * rows * hid
        ),
        compiler_params=pltpu.CompilerParams(vmem_limit_bytes=16 << 20),
        name="mlp",
    )(*xs, w_gate, w_up, w_down)


def shifted(x, axis, by):
    count = lax.axis_size(axis)
    return lax.ppermute(x, axis, [(i, (i + by) % count) for i in range(count)])


def routing(routes, experts, capacity, zy_count):
    part_rows, top_count = routes.shape
    chosen = routes.reshape(part_rows * top_count)
    order = jnp.arange(part_rows * top_count, dtype=jnp.int32)
    earlier = (chosen[:, None] == chosen[None, :]) & (order[None, :] < order[:, None])
    rank = jnp.sum(earlier.astype(jnp.int32), axis=1)
    away = (chosen % 2) ^ lax.axis_index(CORE)
    slots = away * (zy_count * capacity) + (chosen // 2) * capacity + rank
    slot_ids = jnp.arange(experts * capacity, dtype=jnp.int32)
    hit = (slots[:, None] == slot_ids[None, :]).astype(jnp.bfloat16)
    return hit.reshape(part_rows, top_count, experts * capacity)


def experts_part(moe_tokens, moe_gain, routes, route_weights, w_gate, w_up, w_down, queries):
    n_rows = moe_tokens.shape[0]
    top_count = routes.shape[1]
    quarters = lax.axis_size("tp")
    part_rows = n_rows // quarters
    experts = lax.axis_size(EP)
    zy_count = lax.axis_size(ZY)
    capacity = (3 * top_count * part_rows + 2 * experts - 1) // (2 * experts)
    my_part = lax.axis_index("tp")
    first = my_part * part_rows
    own_rows = lax.dynamic_slice_in_dim(moe_tokens, first, part_rows, 0)
    normed = rms_norm(own_rows.astype(jnp.float32), moe_gain).astype(jnp.bfloat16)
    own_routes = lax.dynamic_slice_in_dim(routes, first, part_rows, 0)
    own_weights = lax.dynamic_slice_in_dim(route_weights, first, part_rows, 0)
    hit = routing(own_routes, experts, capacity, zy_count)
    send = jnp.sum(hit, axis=1)
    half = zy_count * capacity

    def outgoing(cols):
        return jnp.einsum("rs,rd->sd", cols, normed, preferred_element_type=jnp.float32).astype(jnp.bfloat16)

    near = outgoing(send[:, :half])
    far = shifted(outgoing(send[:, half:]), CORE, 1)

    def dispatch(rows):
        blocks = rows.reshape(zy_count, -1, 128)
        return lax.all_to_all(blocks, ZY, 0, 0, tiled=True).reshape(rows.shape)

    def spread(rows):
        return [rows, shifted(rows, "tp", 1), shifted(rows, "tp", -1), shifted(rows, "tp", 2)]

    def total(parts):
        back = [parts[0], shifted(parts[1], "tp", -1), shifted(parts[2], "tp", 1), shifted(parts[3], "tp", 2)]
        whole = back[0]
        for part in back[1:]:
            whole = whole + part.astype(jnp.float32)
        return whole.astype(jnp.bfloat16)

    near, queries = lax.optimization_barrier((near, queries))
    near_x = spread(dispatch(near))
    far_x = spread(dispatch(far))
    near_y = mlp(near_x, w_gate[0], w_up[0], w_down[0])
    far_y = mlp(far_x, w_gate[0], w_up[0], w_down[0])
    near_back = dispatch(total(near_y))
    far_back = shifted(dispatch(total(far_y)), CORE, 1)
    picked = jnp.einsum("rks,sd->rkd", hit[..., :half], near_back, preferred_element_type=jnp.float32) + jnp.einsum(
        "rks,sd->rkd", hit[..., half:], far_back, preferred_element_type=jnp.float32
    )
    return jnp.sum(picked * own_weights[:, :, None], axis=1).astype(jnp.bfloat16), queries


def on_device(
    queries,
    kv_latent,
    rope_key,
    latent_gain,
    w_key_up,
    w_value_up,
    query_gain,
    key_gain,
    rope_gain,
    out_gain,
    moe_tokens,
    moe_gain,
    routes,
    route_weights,
    w_gate,
    w_up,
    w_down,
):
    tok_rows = queries.shape[0]
    index = lax.axis_index(EP)
    positions = index * tok_rows + jnp.arange(tok_rows, dtype=jnp.int32)
    moe_out, queries = experts_part(
        moe_tokens, moe_gain, routes, route_weights, w_gate, w_up, w_down, queries
    )
    keys, own_queries = prepare(
        queries, kv_latent, rope_key, latent_gain, w_key_up, w_value_up, query_gain, key_gain, rope_gain, positions
    )
    keys = lax.all_gather(keys, "ep_0", axis=0, tiled=True)
    all_queries = lax.all_gather(own_queries, YC, axis=0, tiled=True)
    at = jnp.stack([lax.axis_index("ep_0"), lax.axis_index(YC)]).astype(jnp.int32)
    parts = flash(at, all_queries, keys, lax.axis_size("ep_0"), query_gain.shape[0] ** -0.5)
    parts = lax.all_to_all(parts, YC, 0, 0, tiled=True)
    attended = finish(parts, out_gain, lax.axis_size(YC), tok_rows)
    return (attended, moe_out)


def solution(mesh):
    finer = Mesh(mesh.devices.reshape(8, 4, 2, mesh.shape["tp"]), ("ep_0", "ep_1", "ep_2", "tp"))
    placed = (
        P(EP, "tp"),
        P(EP, None),
        P(EP, None),
        P(),
        P(None, "tp"),
        P(None, "tp"),
        P(),
        P(),
        P(),
        P(),
        P(EP, None),
        P(),
        P(EP, None),
        P(EP, None),
        P(EP, None, "tp"),
        P(EP, None, "tp"),
        P(EP, "tp", None),
    )
    return jax.shard_map(
        on_device,
        mesh=finer,
        in_specs=placed,
        out_specs=(P(EP, "tp"), P(EP_TP, None)),
        check_vma=False,
    )
```

```python
import functools

import jax
import jax.numpy as jnp
from jax import lax
from jax.experimental import pallas as pl
from jax.experimental.pallas import tpu as pltpu
from jax.sharding import Mesh
from jax.sharding import PartitionSpec as P


ZY = ("ep_0", "ep_1")
CORE = "ep_2"
YC = ("ep_1", "ep_2")
EP = ("ep_0", "ep_1", "ep_2")
EP_TP = ("ep_0", "ep_1", "ep_2", "tp")

EPS = 1e-06
THETA = 500000.0
LOG2E = 1.4426950408889634


def rms_norm(values, norm_gain):
    return values * lax.rsqrt(jnp.mean(values * values, axis=-1, keepdims=True) + EPS) * norm_gain


def in_hbm(x):
    return pltpu.with_memory_space_constraint(x, pltpu.HBM)


def swap_halves(v):
    lane = lax.broadcasted_iota(jnp.int32, v.shape, 1)
    return jnp.where(lane % 64 < 32, pltpu.roll(v, 96, 1), pltpu.roll(v, 32, 1))


def prepare_body(*refs):
    sources = refs[:11]
    keys_out, queries_out = refs[11:13]
    queries_ref, latent_ref, rope_ref, latent_gain, wk_ref, wv_ref, query_gain, key_gain, rope_gain, cos_ref, sin_ref = (
        refs[13:24]
    )
    sem = refs[24]
    copies = [pltpu.make_async_copy(s, d, sem.at[k]) for k, (s, d) in enumerate(zip(sources, refs[13:24]))]
    for copy in copies:
        copy.start()
    for copy in copies:
        copy.wait()
    rows = latent_ref.shape[0]
    half = rows // 2
    heads = wk_ref.shape[1] // 128
    latent = rms_norm(latent_ref[...].astype(jnp.float32), latent_gain[...]).astype(jnp.bfloat16)
    keys = jnp.dot(latent, wk_ref[...], preferred_element_type=jnp.float32)
    values = jnp.dot(latent, wv_ref[...], preferred_element_type=jnp.float32)
    for h in range(heads):
        cols = slice(h * 128, (h + 1) * 128)
        keys_out[h * rows : (h + 1) * rows, :] = rms_norm(keys[:, cols], key_gain[...]).astype(jnp.bfloat16)
        keys_out[(heads + h) * rows : (heads + h + 1) * rows, :] = values[:, cols].astype(jnp.bfloat16)
    cos = cos_ref[...]
    sin = sin_ref[...]
    lane = lax.broadcasted_iota(jnp.int32, (half, 128), 1)
    rope = rms_norm(rope_ref[...].astype(jnp.float32), rope_gain[...])
    rope = jnp.concatenate([rope[:half], rope[half:]], axis=1)
    cos_k = jnp.where(lane < 64, cos[:half], cos[half:])
    sin_k = jnp.where(lane < 64, sin[:half], sin[half:])
    keys_out[2 * heads * rows :, :] = (rope * cos_k + swap_halves(rope) * sin_k).astype(jnp.bfloat16)
    ropes = []
    for h in range(heads):
        query = rms_norm(queries_ref[:, h * 192 : (h + 1) * 192].astype(jnp.float32), query_gain[...])
        queries_out[h * rows : (h + 1) * rows, :] = query[:, :128].astype(jnp.bfloat16)
        ropes.append(query[:, 128:])
    rope = jnp.concatenate(ropes, axis=1)
    queries_out[heads * rows :, :] = (rope * cos + swap_halves(rope) * sin).astype(jnp.bfloat16)


def prepare(queries, kv_latent, rope_key, latent_gain, w_key_up, w_value_up, query_gain, key_gain, rope_gain, positions):
    rows = queries.shape[0]
    rope_dim = rope_key.shape[1]
    freqs = 1.0 / THETA ** (jnp.arange(0, rope_dim, 2, dtype=jnp.float32) / rope_dim)
    lane = jnp.arange(128, dtype=jnp.int32)
    angles = positions.astype(jnp.float32)[:, None] * jnp.tile(freqs, 4)[None, :]
    sign = jnp.where(lane % 64 < 32, -1.0, 1.0)[None, :]
    args = (
        queries, kv_latent, rope_key, latent_gain.reshape(1, -1), w_key_up, w_value_up, query_gain.reshape(1, -1),
        key_gain.reshape(1, -1), rope_gain.reshape(1, -1), jnp.cos(angles), jnp.sin(angles) * sign,
    )
    return pl.pallas_call(
        prepare_body,
        in_specs=[pl.BlockSpec(memory_space=pltpu.HBM)] * len(args),
        out_specs=[pl.BlockSpec(memory_space=pltpu.VMEM)] * 2,
        scratch_shapes=[pltpu.VMEM(a.shape, a.dtype) for a in args] + [pltpu.SemaphoreType.DMA((len(args),))],
        out_shape=[
            jax.ShapeDtypeStruct((rows * 9 // 2, 128), jnp.bfloat16),
            jax.ShapeDtypeStruct((rows * 3, 128), jnp.bfloat16),
        ],
        cost_estimate=pl.CostEstimate(flops=rows * 512 * 512 * 2, bytes_accessed=2 << 20, transcendentals=0),
        compiler_params=pltpu.CompilerParams(vmem_limit_bytes=16 << 20),
        name="prepare",
    )(*[in_hbm(a) for a in args])


def flash_body(groups, rows, scale, pieces, at_ref, *refs):
    q_hbm = refs[:pieces]
    kv_hbm, out_ref, kt_ref, vt_ref, all_q_ref, kv_ref, sem = refs[pieces:]
    tile = pl.program_id(0)
    group = at_ref[0]
    place = at_ref[1]
    heads = 2
    half = rows // 2
    per = kv_ref.shape[0] // groups

    @pl.when(tile == 0)
    def _():
        lane = lax.broadcasted_iota(jnp.int32, (rows, 128), 1)
        copies = []
        for g in range(groups):
            part = pl.ds(g * per, per)
            copies.append(pltpu.make_async_copy(kv_hbm.at[part], kv_ref.at[part], sem.at[g]))
        first = 0
        for k, piece in enumerate(q_hbm):
            part = pl.ds(first, piece.shape[0])
            copies.append(pltpu.make_async_copy(piece, all_q_ref.at[part], sem.at[groups + k]))
            first += piece.shape[0]
        for copy in copies:
            copy.start()
        for g in range(groups):
            copies[g].wait()
            base = g * per
            seen = jnp.where(g <= group, 1.0, 0.0).astype(jnp.float32)
            rope = kv_ref[base + 2 * heads * rows : base + per, :].astype(jnp.float32)
            turned = pltpu.roll(rope, 64, 1)
            low = jnp.where(lane < 64, jnp.concatenate([rope, turned], axis=0), 0.0).astype(jnp.bfloat16)
            high = jnp.where(lane >= 64, jnp.concatenate([turned, rope], axis=0), 0.0).astype(jnp.bfloat16)
            for h in range(heads):
                kt_ref[g * heads + h, :, :128] = kv_ref[base + h * rows : base + (h + 1) * rows, :]
                kt_ref[g * heads + h, :, 128:] = low if h == 0 else high
                vals = kv_ref[base + (heads + h) * rows : base + (heads + h + 1) * rows, :].astype(jnp.float32)
                vt_ref[g * heads + h, :, :128] = (vals * seen).astype(jnp.bfloat16)
                vt_ref[g * heads + h, :, 128:] = jnp.full((rows, 128), seen, jnp.float32).astype(jnp.bfloat16)

        for copy in copies[groups:]:
            copy.wait()

    q_ref = all_q_ref.at[pl.ds(pl.multiple_of(tile * 3 * rows, 3 * rows), 3 * rows)]
    q_rope = q_ref[heads * rows :, :]
    sums = []
    for h in range(heads):
        query = jnp.concatenate([q_ref[h * rows : (h + 1) * rows, :], q_rope], axis=1)
        total = None
        for k in range(groups):
            at = ((group + k) % groups) * heads + h
            scores = lax.dot_general(
                query, kt_ref[at], (((1,), (1,)), ((), ())), preferred_element_type=jnp.float32
            )
            soft = jnp.exp2(scores * (scale * LOG2E))
            if k == 0:
                qi = lax.broadcasted_iota(jnp.int32, soft.shape, 0) + (at_ref[2 + tile] - place) * rows
                ki = lax.broadcasted_iota(jnp.int32, soft.shape, 1)
                soft = jnp.where(qi >= ki, soft, 0.0)
            part = jnp.dot(soft.astype(jnp.bfloat16), vt_ref[at], preferred_element_type=jnp.float32)
            total = part if total is None else total + part
        out_ref[h * rows : (h + 1) * rows, :] = total[:, :128].astype(jnp.bfloat16)
        for t in range(2):
            den = total[t * half : (t + 1) * half, 128:]
            ri = lax.broadcasted_iota(jnp.int32, den.shape, 0)
            ci = lax.broadcasted_iota(jnp.int32, den.shape, 1)
            sums.append(jnp.sum(jnp.where(ri == ci, den, 0.0), axis=0, keepdims=True))
    sums = jnp.concatenate(sums + [jnp.zeros((4, 128), jnp.float32)], axis=0)
    high = sums.astype(jnp.bfloat16).astype(jnp.float32)
    low = sums - high
    out_ref[heads * rows :, :] = jnp.concatenate([high, low], axis=0).astype(jnp.bfloat16)


def flash(at, pieces, keys, groups, scale):
    rows = keys.shape[0] // groups * 2 // 9
    q_rows = sum(p.shape[0] for p in pieces)
    tiles = q_rows // (3 * rows)
    out_rows = 2 * rows + 16
    grid_spec = pltpu.PrefetchScalarGridSpec(
        num_scalar_prefetch=1,
        grid=(tiles,),
        in_specs=[
            pl.BlockSpec(memory_space=pltpu.HBM),
        ]
        * (len(pieces) + 1),
        out_specs=pl.BlockSpec((out_rows, 128), lambda s, i: (i[2 + s], 0)),
        scratch_shapes=[
            pltpu.VMEM((2 * groups, rows, 256), jnp.bfloat16),
            pltpu.VMEM((2 * groups, rows, 256), jnp.bfloat16),
            pltpu.VMEM((q_rows, 128), jnp.bfloat16),
            pltpu.VMEM(keys.shape, jnp.bfloat16),
            pltpu.SemaphoreType.DMA((groups + len(pieces),)),
        ],
    )
    pairs = 2 * rows * rows * groups * tiles
    return pl.pallas_call(
        functools.partial(flash_body, groups, rows, scale, len(pieces)),
        grid_spec=grid_spec,
        out_shape=jax.ShapeDtypeStruct((tiles * out_rows, 128), jnp.bfloat16),
        cost_estimate=pl.CostEstimate(flops=pairs * 1024, bytes_accessed=4 << 20, transcendentals=pairs),
        compiler_params=pltpu.CompilerParams(dimension_semantics=("arbitrary",), vmem_limit_bytes=24 << 20),
        name="flash",
    )(at, *[in_hbm(p) for p in pieces], in_hbm(keys))


def finish_body(count, in_ref, gain_ref, out_ref):
    per = in_ref.shape[0] // count
    rows = out_ref.shape[0]
    half = rows // 2
    total = in_ref[:per, :].astype(jnp.float32)
    for k in range(1, count):
        total = total + in_ref[k * per : (k + 1) * per, :].astype(jnp.float32)
    sums = total[2 * rows : 2 * rows + 8] + total[2 * rows + 8 : 2 * rows + 16]
    ri = lax.broadcasted_iota(jnp.int32, (half, 128), 0)
    ci = lax.broadcasted_iota(jnp.int32, (half, 128), 1)
    for h in range(2):
        for t in range(2):
            den = jnp.sum(jnp.where(ri == ci, sums[2 * h + t : 2 * h + t + 1], 0.0), axis=1, keepdims=True)
            mixed = total[h * rows + t * half : h * rows + (t + 1) * half] / den
            out_ref[t * half : (t + 1) * half, h * 128 : (h + 1) * 128] = rms_norm(mixed, gain_ref[...]).astype(
                jnp.bfloat16
            )


def finish(parts, out_gain, count, rows):
    whole = pl.BlockSpec(memory_space=pltpu.VMEM)
    return pl.pallas_call(
        functools.partial(finish_body, count),
        in_specs=[whole, whole],
        out_specs=whole,
        out_shape=jax.ShapeDtypeStruct((rows, 256), jnp.bfloat16),
        compiler_params=pltpu.CompilerParams(vmem_limit_bytes=16 << 20),
        name="finish",
    )(parts, out_gain.reshape(1, -1))


def mlp_body(pieces, *refs):
    x_refs = refs[:pieces]
    wg_ref, wu_ref, wd_ref = refs[pieces : pieces + 3]
    out_refs = refs[pieces + 3 :]
    x = jnp.concatenate([r[...] for r in x_refs], axis=0)
    gate = jnp.dot(x, wg_ref[...], preferred_element_type=jnp.float32)
    up = jnp.dot(x, wu_ref[...], preferred_element_type=jnp.float32)
    hidden = (gate / (1.0 + jnp.exp(-gate)) * up).astype(jnp.bfloat16)
    y = jnp.dot(hidden, wd_ref[...], preferred_element_type=jnp.float32)
    first = 0
    for ref in out_refs:
        ref[...] = y[first : first + ref.shape[0]].astype(ref.dtype)
        first += ref.shape[0]


def mlp(xs, w_gate, w_up, w_down):
    rows = sum(x.shape[0] for x in xs)
    dim, hid = w_gate.shape
    whole = pl.BlockSpec(memory_space=pltpu.VMEM)
    dtypes = [jnp.float32] + [jnp.bfloat16] * (len(xs) - 1)
    return pl.pallas_call(
        functools.partial(mlp_body, len(xs)),
        in_specs=[whole] * (len(xs) + 3),
        out_specs=[whole] * len(xs),
        out_shape=[jax.ShapeDtypeStruct(x.shape, d) for x, d in zip(xs, dtypes)],
        cost_estimate=pl.CostEstimate(
            flops=2 * rows * dim * hid * 3, bytes_accessed=3 * dim * hid * 2, transcendentals=rows * hid
        ),
        compiler_params=pltpu.CompilerParams(vmem_limit_bytes=16 << 20),
        name="mlp",
    )(*xs, w_gate, w_up, w_down)


def shifted(x, axis, by):
    count = lax.axis_size(axis)
    return lax.ppermute(x, axis, [(i, (i + by) % count) for i in range(count)])


def send_body(capacity, at_ref, routes_ref, tokens_ref, gain_ref, near_out, far_out, hits_out):
    core = at_ref[1]
    rows = tokens_ref.shape[0]
    lane = lax.broadcasted_iota(jnp.int32, (rows, 128), 1)
    normed = rms_norm(tokens_ref[...].astype(jnp.float32), gain_ref[...]).astype(jnp.bfloat16)
    chosen = [routes_ref[:, k : k + 1] for k in range(2)]
    named = [(c == lane).astype(jnp.float32) for c in chosen]
    before = lax.broadcasted_iota(jnp.int32, (rows, rows), 1) < lax.broadcasted_iota(jnp.int32, (rows, rows), 0)
    count = jnp.dot(
        before.astype(jnp.float32).astype(jnp.bfloat16),
        (named[0] + named[1]).astype(jnp.bfloat16),
        preferred_element_type=jnp.float32,
    )
    sends = [jnp.zeros((rows, 128), jnp.float32), jnp.zeros((rows, 128), jnp.float32)]
    for k in range(2):
        rank = jnp.sum(count * named[k], axis=1, keepdims=True).astype(jnp.int32)
        away = (chosen[k] & 1) ^ core
        slot = (chosen[k] >> 1) * capacity + rank
        for side in range(2):
            hit = ((slot == lane) & (away == side)).astype(jnp.float32)
            hits_out[side, k] = hit.astype(jnp.bfloat16)
            sends[side] = sends[side] + hit
    for side, ref in enumerate((near_out, far_out)):
        moved = lax.dot_general(
            sends[side].astype(jnp.bfloat16), normed, (((0,), (0,)), ((), ())), preferred_element_type=jnp.float32
        )
        ref[...] = moved[: ref.shape[0]].astype(jnp.bfloat16)


def send_rows(part, moe_tokens, moe_gain, routes, part_rows, capacity, half):
    dim = moe_tokens.shape[1]
    at = jnp.stack([part, lax.axis_index(CORE)]).astype(jnp.int32)
    grid_spec = pltpu.PrefetchScalarGridSpec(
        num_scalar_prefetch=1,
        grid=(1,),
        in_specs=[
            pl.BlockSpec((part_rows, 2), lambda s, i: (i[0], 0)),
            pl.BlockSpec((part_rows, dim), lambda s, i: (i[0], 0)),
            pl.BlockSpec((1, dim), lambda s, i: (0, 0)),
        ],
        out_specs=[
            pl.BlockSpec((half, dim), lambda s, i: (0, 0)),
            pl.BlockSpec((half, dim), lambda s, i: (0, 0)),
            pl.BlockSpec((2, 2, part_rows, 128), lambda s, i: (0, 0, 0, 0)),
        ],
    )
    return pl.pallas_call(
        functools.partial(send_body, capacity),
        grid_spec=grid_spec,
        out_shape=[
            jax.ShapeDtypeStruct((half, dim), jnp.bfloat16),
            jax.ShapeDtypeStruct((half, dim), jnp.bfloat16),
            jax.ShapeDtypeStruct((2, 2, part_rows, 128), jnp.bfloat16),
        ],
        compiler_params=pltpu.CompilerParams(vmem_limit_bytes=16 << 20),
        name="send",
    )(at, in_hbm(routes), in_hbm(moe_tokens), in_hbm(moe_gain.reshape(1, -1)))


def experts_part(moe_tokens, moe_gain, routes, route_weights, w_gate, w_up, w_down, queries, attend):
    n_rows = moe_tokens.shape[0]
    top_count = routes.shape[1]
    quarters = lax.axis_size("tp")
    part_rows = n_rows // quarters
    experts = lax.axis_size(EP)
    zy_count = lax.axis_size(ZY)
    capacity = (3 * top_count * part_rows + 2 * experts - 1) // (2 * experts)
    my_part = lax.axis_index("tp")
    own_weights = lax.dynamic_slice_in_dim(route_weights, my_part * part_rows, part_rows, 0)
    half = zy_count * capacity
    near, far, hits = send_rows(my_part, moe_tokens, moe_gain, routes, part_rows, capacity, half)
    far = shifted(far, CORE, 1)

    def dispatch(rows):
        blocks = rows.reshape(zy_count, -1, 128)
        return lax.all_to_all(blocks, ZY, 0, 0, tiled=True).reshape(rows.shape)

    def spread(rows):
        return [rows, shifted(rows, "tp", 1), shifted(rows, "tp", -1), shifted(rows, "tp", 2)]

    def total(parts):
        back = [parts[0], shifted(parts[1], "tp", -1), shifted(parts[2], "tp", 1), shifted(parts[3], "tp", 2)]
        whole = back[0]
        for part in back[1:]:
            whole = whole + part.astype(jnp.float32)
        return whole.astype(jnp.bfloat16)

    near_in = dispatch(near)
    far_in = dispatch(far)
    near_x = spread(near_in)
    far_x = spread(far_in)
    near_y = mlp(near_x, w_gate[0], w_up[0], w_down[0])
    far_y = mlp(far_x, w_gate[0], w_up[0], w_down[0])
    parts = attend(queries)
    near_sum = total(near_y)
    far_sum = total(far_y)
    near_back = dispatch(near_sum)
    far_back = dispatch(far_sum)
    far_back = shifted(far_back, CORE, 1)
    mixed = jnp.zeros((part_rows, near_back.shape[1]), jnp.float32)
    for k in range(top_count):
        picked = jnp.dot(hits[0, k, :, :half], near_back, preferred_element_type=jnp.float32) + jnp.dot(
            hits[1, k, :, :half], far_back, preferred_element_type=jnp.float32
        )
        mixed = mixed + picked * own_weights[:, k : k + 1]
    return mixed.astype(jnp.bfloat16), parts


def on_device(
    queries,
    kv_latent,
    rope_key,
    latent_gain,
    w_key_up,
    w_value_up,
    query_gain,
    key_gain,
    rope_gain,
    out_gain,
    moe_tokens,
    moe_gain,
    routes,
    route_weights,
    w_gate,
    w_up,
    w_down,
):
    tok_rows = queries.shape[0]
    index = lax.axis_index(EP)
    positions = index * tok_rows + jnp.arange(tok_rows, dtype=jnp.int32)

    def attend(raw_queries):
        keys, own = prepare(
            raw_queries, kv_latent, rope_key, latent_gain, w_key_up, w_value_up, query_gain, key_gain, rope_gain, positions
        )
        keys = lax.all_gather(keys, "ep_0", axis=0, tiled=True)
        pair = jnp.concatenate([own, shifted(own, CORE, 1)], axis=0)
        shifts = (0, 1, 3, 2)
        pieces = [pair] + [shifted(pair, "ep_1", s) for s in shifts[1:]]
        row = lax.axis_index("ep_1")
        core = lax.axis_index(CORE)
        places = [((row - s) & 3) * 2 + (core ^ away) for s in shifts for away in (0, 1)]
        at = jnp.stack([lax.axis_index("ep_0"), row * 2 + core] + places).astype(jnp.int32)
        return flash(at, pieces, keys, lax.axis_size("ep_0"), query_gain.shape[0] ** -0.5)

    moe_out, parts = experts_part(
        moe_tokens, moe_gain, routes, route_weights, w_gate, w_up, w_down, queries, attend
    )
    parts = lax.psum_scatter(parts, YC, scatter_dimension=0, tiled=True)
    attended = finish(parts, out_gain, 1, tok_rows)
    return (attended, moe_out)


def solution(mesh):
    finer = Mesh(mesh.devices.reshape(8, 4, 2, mesh.shape["tp"]), ("ep_0", "ep_1", "ep_2", "tp"))
    placed = (
        P(EP, "tp"),
        P(EP, None),
        P(EP, None),
        P(),
        P(None, "tp"),
        P(None, "tp"),
        P(),
        P(),
        P(),
        P(),
        P(EP, None),
        P(),
        P(EP, None),
        P(EP, None),
        P(EP, None, "tp"),
        P(EP, None, "tp"),
        P(EP, "tp", None),
    )

    return jax.shard_map(
        on_device,
        mesh=finer,
        in_specs=placed,
        out_specs=(P(EP, "tp"), P(EP_TP, None)),
        check_vma=False,
    )
```

```python
import functools

import jax
import jax.numpy as jnp
from jax import lax
from jax.experimental import pallas as pl
from jax.experimental.pallas import tpu as pltpu
from jax.sharding import Mesh
from jax.sharding import PartitionSpec as P


ZY = ("ep_0", "ep_1")
CORE = "ep_2"
YC = ("ep_1", "ep_2")
EP = ("ep_0", "ep_1", "ep_2")
EP_TP = ("ep_0", "ep_1", "ep_2", "tp")

EPS = 1e-06
THETA = 500000.0
LOG2E = 1.4426950408889634


def rms_norm(values, norm_gain):
    return values * lax.rsqrt(jnp.mean(values * values, axis=-1, keepdims=True) + EPS) * norm_gain


def in_hbm(x):
    return pltpu.with_memory_space_constraint(x, pltpu.HBM)


def swap_halves(v):
    lane = lax.broadcasted_iota(jnp.int32, v.shape, 1)
    return jnp.where(lane % 64 < 32, pltpu.roll(v, 96, 1), pltpu.roll(v, 32, 1))


def prepare_body(*refs):
    sources = refs[:11]
    keys_out, queries_out = refs[11:13]
    queries_ref, latent_ref, rope_ref, latent_gain, wk_ref, wv_ref, query_gain, key_gain, rope_gain, cos_ref, sin_ref = (
        refs[13:24]
    )
    sem = refs[24]
    copies = [pltpu.make_async_copy(s, d, sem.at[k]) for k, (s, d) in enumerate(zip(sources, refs[13:24]))]
    for copy in copies:
        copy.start()
    for copy in copies:
        copy.wait()
    rows = latent_ref.shape[0]
    half = rows // 2
    heads = wk_ref.shape[1] // 128
    latent = rms_norm(latent_ref[...].astype(jnp.float32), latent_gain[...]).astype(jnp.bfloat16)
    keys = jnp.dot(latent, wk_ref[...], preferred_element_type=jnp.float32)
    values = jnp.dot(latent, wv_ref[...], preferred_element_type=jnp.float32)
    for h in range(heads):
        cols = slice(h * 128, (h + 1) * 128)
        keys_out[h * rows : (h + 1) * rows, :] = rms_norm(keys[:, cols], key_gain[...]).astype(jnp.bfloat16)
        keys_out[(heads + h) * rows : (heads + h + 1) * rows, :] = values[:, cols].astype(jnp.bfloat16)
    cos = cos_ref[...]
    sin = sin_ref[...]
    lane = lax.broadcasted_iota(jnp.int32, (half, 128), 1)
    rope = rms_norm(rope_ref[...].astype(jnp.float32), rope_gain[...])
    rope = jnp.concatenate([rope[:half], rope[half:]], axis=1)
    cos_k = jnp.where(lane < 64, cos[:half], cos[half:])
    sin_k = jnp.where(lane < 64, sin[:half], sin[half:])
    keys_out[2 * heads * rows :, :] = (rope * cos_k + swap_halves(rope) * sin_k).astype(jnp.bfloat16)
    ropes = []
    for h in range(heads):
        query = rms_norm(queries_ref[:, h * 192 : (h + 1) * 192].astype(jnp.float32), query_gain[...])
        queries_out[h * rows : (h + 1) * rows, :] = query[:, :128].astype(jnp.bfloat16)
        ropes.append(query[:, 128:])
    rope = jnp.concatenate(ropes, axis=1)
    queries_out[heads * rows :, :] = (rope * cos + swap_halves(rope) * sin).astype(jnp.bfloat16)


def prepare(queries, kv_latent, rope_key, latent_gain, w_key_up, w_value_up, query_gain, key_gain, rope_gain, positions):
    rows = queries.shape[0]
    rope_dim = rope_key.shape[1]
    freqs = 1.0 / THETA ** (jnp.arange(0, rope_dim, 2, dtype=jnp.float32) / rope_dim)
    lane = jnp.arange(128, dtype=jnp.int32)
    angles = positions.astype(jnp.float32)[:, None] * jnp.tile(freqs, 4)[None, :]
    sign = jnp.where(lane % 64 < 32, -1.0, 1.0)[None, :]
    args = (
        queries, kv_latent, rope_key, latent_gain.reshape(1, -1), w_key_up, w_value_up, query_gain.reshape(1, -1),
        key_gain.reshape(1, -1), rope_gain.reshape(1, -1), jnp.cos(angles), jnp.sin(angles) * sign,
    )
    return pl.pallas_call(
        prepare_body,
        in_specs=[pl.BlockSpec(memory_space=pltpu.HBM)] * len(args),
        out_specs=[pl.BlockSpec(memory_space=pltpu.VMEM)] * 2,
        scratch_shapes=[pltpu.VMEM(a.shape, a.dtype) for a in args] + [pltpu.SemaphoreType.DMA((len(args),))],
        out_shape=[
            jax.ShapeDtypeStruct((rows * 9 // 2, 128), jnp.bfloat16),
            jax.ShapeDtypeStruct((rows * 3, 128), jnp.bfloat16),
        ],
        cost_estimate=pl.CostEstimate(flops=rows * 512 * 512 * 2, bytes_accessed=2 << 20, transcendentals=0),
        compiler_params=pltpu.CompilerParams(vmem_limit_bytes=16 << 20),
        name="prepare",
    )(*[in_hbm(a) for a in args])


def flash_body(groups, rows, scale, pieces, at_ref, *refs):
    q_hbm = refs[:pieces]
    kv_hbm, out_ref, kt_ref, vt_ref, all_q_ref, kv_ref, sem = refs[pieces:]
    tile = pl.program_id(0)
    group = at_ref[0]
    place = at_ref[1]
    heads = 2
    half = rows // 2
    per = kv_ref.shape[0] // groups

    @pl.when(tile == 0)
    def _():
        lane = lax.broadcasted_iota(jnp.int32, (rows, 128), 1)
        copies = []
        for g in range(groups):
            part = pl.ds(g * per, per)
            copies.append(pltpu.make_async_copy(kv_hbm.at[part], kv_ref.at[part], sem.at[g]))
        first = 0
        for k, piece in enumerate(q_hbm):
            part = pl.ds(first, piece.shape[0])
            copies.append(pltpu.make_async_copy(piece, all_q_ref.at[part], sem.at[groups + k]))
            first += piece.shape[0]
        for copy in copies:
            copy.start()
        for g in range(groups):
            copies[g].wait()
            base = g * per
            seen = jnp.where(g <= group, 1.0, 0.0).astype(jnp.float32)
            rope = kv_ref[base + 2 * heads * rows : base + per, :].astype(jnp.float32)
            turned = pltpu.roll(rope, 64, 1)
            low = jnp.where(lane < 64, jnp.concatenate([rope, turned], axis=0), 0.0).astype(jnp.bfloat16)
            high = jnp.where(lane >= 64, jnp.concatenate([turned, rope], axis=0), 0.0).astype(jnp.bfloat16)
            for h in range(heads):
                kt_ref[g * heads + h, :, :128] = kv_ref[base + h * rows : base + (h + 1) * rows, :]
                kt_ref[g * heads + h, :, 128:] = low if h == 0 else high
                vals = kv_ref[base + (heads + h) * rows : base + (heads + h + 1) * rows, :].astype(jnp.float32)
                vt_ref[g * heads + h, :, :128] = (vals * seen).astype(jnp.bfloat16)
                vt_ref[g * heads + h, :, 128:] = jnp.full((rows, 128), seen, jnp.float32).astype(jnp.bfloat16)

        for copy in copies[groups:]:
            copy.wait()

    q_ref = all_q_ref.at[pl.ds(pl.multiple_of(tile * 3 * rows, 3 * rows), 3 * rows)]
    q_rope = q_ref[heads * rows :, :]
    sums = []
    for h in range(heads):
        query = jnp.concatenate([q_ref[h * rows : (h + 1) * rows, :], q_rope], axis=1)
        total = None
        for k in range(groups):
            at = ((group + k) % groups) * heads + h
            scores = lax.dot_general(
                query, kt_ref[at], (((1,), (1,)), ((), ())), preferred_element_type=jnp.float32
            )
            soft = jnp.exp2(scores * (scale * LOG2E))
            if k == 0:
                qi = lax.broadcasted_iota(jnp.int32, soft.shape, 0) + (at_ref[2 + tile] - place) * rows
                ki = lax.broadcasted_iota(jnp.int32, soft.shape, 1)
                soft = jnp.where(qi >= ki, soft, 0.0)
            part = jnp.dot(soft.astype(jnp.bfloat16), vt_ref[at], preferred_element_type=jnp.float32)
            total = part if total is None else total + part
        out_ref[h * rows : (h + 1) * rows, :] = total[:, :128].astype(jnp.bfloat16)
        for t in range(2):
            den = total[t * half : (t + 1) * half, 128:]
            ri = lax.broadcasted_iota(jnp.int32, den.shape, 0)
            ci = lax.broadcasted_iota(jnp.int32, den.shape, 1)
            sums.append(jnp.sum(jnp.where(ri == ci, den, 0.0), axis=0, keepdims=True))
    sums = jnp.concatenate(sums + [jnp.zeros((4, 128), jnp.float32)], axis=0)
    high = sums.astype(jnp.bfloat16).astype(jnp.float32)
    low = sums - high
    out_ref[heads * rows :, :] = jnp.concatenate([high, low], axis=0).astype(jnp.bfloat16)


def flash(at, pieces, keys, groups, scale):
    rows = keys.shape[0] // groups * 2 // 9
    q_rows = sum(p.shape[0] for p in pieces)
    tiles = q_rows // (3 * rows)
    out_rows = 2 * rows + 16
    grid_spec = pltpu.PrefetchScalarGridSpec(
        num_scalar_prefetch=1,
        grid=(tiles,),
        in_specs=[
            pl.BlockSpec(memory_space=pltpu.HBM),
        ]
        * (len(pieces) + 1),
        out_specs=pl.BlockSpec((out_rows, 128), lambda s, i: (i[2 + s], 0)),
        scratch_shapes=[
            pltpu.VMEM((2 * groups, rows, 256), jnp.bfloat16),
            pltpu.VMEM((2 * groups, rows, 256), jnp.bfloat16),
            pltpu.VMEM((q_rows, 128), jnp.bfloat16),
            pltpu.VMEM(keys.shape, jnp.bfloat16),
            pltpu.SemaphoreType.DMA((groups + len(pieces),)),
        ],
    )
    pairs = 2 * rows * rows * groups * tiles
    return pl.pallas_call(
        functools.partial(flash_body, groups, rows, scale, len(pieces)),
        grid_spec=grid_spec,
        out_shape=jax.ShapeDtypeStruct((tiles * out_rows, 128), jnp.bfloat16),
        cost_estimate=pl.CostEstimate(flops=pairs * 1024, bytes_accessed=4 << 20, transcendentals=pairs),
        compiler_params=pltpu.CompilerParams(dimension_semantics=("arbitrary",), vmem_limit_bytes=24 << 20),
        name="flash",
    )(at, *[in_hbm(p) for p in pieces], in_hbm(keys))


def finish_body(count, in_ref, gain_ref, out_ref):
    per = in_ref.shape[0] // count
    rows = out_ref.shape[0]
    half = rows // 2
    total = in_ref[:per, :].astype(jnp.float32)
    for k in range(1, count):
        total = total + in_ref[k * per : (k + 1) * per, :].astype(jnp.float32)
    sums = total[2 * rows : 2 * rows + 8] + total[2 * rows + 8 : 2 * rows + 16]
    ri = lax.broadcasted_iota(jnp.int32, (half, 128), 0)
    ci = lax.broadcasted_iota(jnp.int32, (half, 128), 1)
    for h in range(2):
        for t in range(2):
            den = jnp.sum(jnp.where(ri == ci, sums[2 * h + t : 2 * h + t + 1], 0.0), axis=1, keepdims=True)
            mixed = total[h * rows + t * half : h * rows + (t + 1) * half] / den
            out_ref[t * half : (t + 1) * half, h * 128 : (h + 1) * 128] = rms_norm(mixed, gain_ref[...]).astype(
                jnp.bfloat16
            )


def finish(parts, out_gain, count, rows):
    whole = pl.BlockSpec(memory_space=pltpu.VMEM)
    return pl.pallas_call(
        functools.partial(finish_body, count),
        in_specs=[whole, whole],
        out_specs=whole,
        out_shape=jax.ShapeDtypeStruct((rows, 256), jnp.bfloat16),
        compiler_params=pltpu.CompilerParams(vmem_limit_bytes=16 << 20),
        name="finish",
    )(parts, out_gain.reshape(1, -1))


def mlp_body(pieces, *refs):
    x_refs = refs[:pieces]
    wg_ref, wu_ref, wd_ref = refs[pieces : pieces + 3]
    out_refs = refs[pieces + 3 :]
    x = jnp.concatenate([r[...] for r in x_refs], axis=0)
    gate = jnp.dot(x, wg_ref[...], preferred_element_type=jnp.float32)
    up = jnp.dot(x, wu_ref[...], preferred_element_type=jnp.float32)
    hidden = (gate / (1.0 + jnp.exp(-gate)) * up).astype(jnp.bfloat16)
    y = jnp.dot(hidden, wd_ref[...], preferred_element_type=jnp.float32)
    first = 0
    for ref in out_refs:
        ref[...] = y[first : first + ref.shape[0]].astype(ref.dtype)
        first += ref.shape[0]


def mlp(xs, w_gate, w_up, w_down):
    rows = sum(x.shape[0] for x in xs)
    dim, hid = w_gate.shape
    whole = pl.BlockSpec(memory_space=pltpu.VMEM)
    dtypes = [jnp.float32] + [jnp.bfloat16] * (len(xs) - 1)
    return pl.pallas_call(
        functools.partial(mlp_body, len(xs)),
        in_specs=[whole] * (len(xs) + 3),
        out_specs=[whole] * len(xs),
        out_shape=[jax.ShapeDtypeStruct(x.shape, d) for x, d in zip(xs, dtypes)],
        cost_estimate=pl.CostEstimate(
            flops=2 * rows * dim * hid * 3, bytes_accessed=3 * dim * hid * 2, transcendentals=rows * hid
        ),
        compiler_params=pltpu.CompilerParams(vmem_limit_bytes=16 << 20),
        name="mlp",
    )(*xs, w_gate, w_up, w_down)


def shifted(x, axis, by):
    count = lax.axis_size(axis)
    return lax.ppermute(x, axis, [(i, (i + by) % count) for i in range(count)])


def send_body(capacity, at_ref, routes_ref, tokens_ref, gain_ref, near_out, far_out, hits_out):
    core = at_ref[1]
    rows = tokens_ref.shape[0]
    lane = lax.broadcasted_iota(jnp.int32, (rows, 128), 1)
    normed = rms_norm(tokens_ref[...].astype(jnp.float32), gain_ref[...]).astype(jnp.bfloat16)
    place = lax.broadcasted_iota(jnp.int32, (rows, routes_ref.shape[1]), 0) + at_ref[0] * rows
    own = place == lax.broadcasted_iota(jnp.int32, place.shape, 1)
    names = routes_ref[...].astype(jnp.float32)
    chosen = [
        jnp.sum(jnp.where(own, names[k : k + 1, :], 0.0), axis=1, keepdims=True).astype(jnp.int32) for k in range(2)
    ]
    named = [(c == lane).astype(jnp.float32) for c in chosen]
    before = lax.broadcasted_iota(jnp.int32, (rows, rows), 1) < lax.broadcasted_iota(jnp.int32, (rows, rows), 0)
    count = jnp.dot(
        before.astype(jnp.float32).astype(jnp.bfloat16),
        (named[0] + named[1]).astype(jnp.bfloat16),
        preferred_element_type=jnp.float32,
    )
    sends = [jnp.zeros((rows, 128), jnp.float32), jnp.zeros((rows, 128), jnp.float32)]
    for k in range(2):
        rank = jnp.sum(count * named[k], axis=1, keepdims=True).astype(jnp.int32)
        away = (chosen[k] & 1) ^ core
        slot = (chosen[k] >> 1) * capacity + rank
        for side in range(2):
            hit = ((slot == lane) & (away == side)).astype(jnp.float32)
            hits_out[side, k] = hit.astype(jnp.bfloat16)
            sends[side] = sends[side] + hit
    for side, ref in enumerate((near_out, far_out)):
        moved = lax.dot_general(
            sends[side].astype(jnp.bfloat16), normed, (((0,), (0,)), ((), ())), preferred_element_type=jnp.float32
        )
        ref[...] = moved[: ref.shape[0]].astype(jnp.bfloat16)


def send_rows(part, moe_tokens, moe_gain, routes, part_rows, capacity, half):
    dim = moe_tokens.shape[1]
    at = jnp.stack([part, lax.axis_index(CORE)]).astype(jnp.int32)
    grid_spec = pltpu.PrefetchScalarGridSpec(
        num_scalar_prefetch=1,
        grid=(1,),
        in_specs=[
            pl.BlockSpec((2, moe_tokens.shape[0]), lambda s, i: (0, 0)),
            pl.BlockSpec((part_rows, dim), lambda s, i: (i[0], 0)),
            pl.BlockSpec((1, dim), lambda s, i: (0, 0)),
        ],
        out_specs=[
            pl.BlockSpec((half, dim), lambda s, i: (0, 0)),
            pl.BlockSpec((half, dim), lambda s, i: (0, 0)),
            pl.BlockSpec((2, 2, part_rows, 128), lambda s, i: (0, 0, 0, 0)),
        ],
    )
    return pl.pallas_call(
        functools.partial(send_body, capacity),
        grid_spec=grid_spec,
        out_shape=[
            jax.ShapeDtypeStruct((half, dim), jnp.bfloat16),
            jax.ShapeDtypeStruct((half, dim), jnp.bfloat16),
            jax.ShapeDtypeStruct((2, 2, part_rows, 128), jnp.bfloat16),
        ],
        compiler_params=pltpu.CompilerParams(vmem_limit_bytes=16 << 20),
        name="send",
    )(at, in_hbm(routes.T), in_hbm(moe_tokens), in_hbm(moe_gain.reshape(1, -1)))


def experts_part(moe_tokens, moe_gain, routes, route_weights, w_gate, w_up, w_down, queries, attend):
    n_rows = moe_tokens.shape[0]
    top_count = routes.shape[1]
    quarters = lax.axis_size("tp")
    part_rows = n_rows // quarters
    experts = lax.axis_size(EP)
    zy_count = lax.axis_size(ZY)
    capacity = (3 * top_count * part_rows + 2 * experts - 1) // (2 * experts)
    my_part = lax.axis_index("tp")
    own_weights = lax.dynamic_slice_in_dim(route_weights, my_part * part_rows, part_rows, 0)
    half = zy_count * capacity
    near, far, hits = send_rows(my_part, moe_tokens, moe_gain, routes, part_rows, capacity, half)
    far = shifted(far, CORE, 1)

    def dispatch(rows):
        blocks = rows.reshape(zy_count, -1, 128)
        return lax.all_to_all(blocks, ZY, 0, 0, tiled=True).reshape(rows.shape)

    def spread(rows):
        return [rows, shifted(rows, "tp", 1), shifted(rows, "tp", -1), shifted(rows, "tp", 2)]

    def total(parts):
        back = [parts[0], shifted(parts[1], "tp", -1), shifted(parts[2], "tp", 1), shifted(parts[3], "tp", 2)]
        whole = back[0]
        for part in back[1:]:
            whole = whole + part.astype(jnp.float32)
        return whole.astype(jnp.bfloat16)

    near_in = dispatch(near)
    far_in = dispatch(far)
    near_x = spread(near_in)
    far_x = spread(far_in)
    near_y = mlp(near_x, w_gate[0], w_up[0], w_down[0])
    far_y = mlp(far_x, w_gate[0], w_up[0], w_down[0])
    parts = attend(queries)
    near_sum = total(near_y)
    far_sum = total(far_y)
    both = jnp.concatenate([s.reshape(zy_count, -1, 128) for s in (near_sum, far_sum)], axis=1)
    both = lax.all_to_all(both, ZY, 0, 0, tiled=True)
    cut = both.shape[1] // 2
    near_back = both[:, :cut].reshape(near_sum.shape)
    far_back = both[:, cut:].reshape(far_sum.shape)
    far_back = shifted(far_back, CORE, 1)
    mixed = jnp.zeros((part_rows, near_back.shape[1]), jnp.float32)
    for k in range(top_count):
        picked = jnp.dot(hits[0, k, :, :half], near_back, preferred_element_type=jnp.float32) + jnp.dot(
            hits[1, k, :, :half], far_back, preferred_element_type=jnp.float32
        )
        mixed = mixed + picked * own_weights[:, k : k + 1]
    return mixed.astype(jnp.bfloat16), parts


def on_device(
    queries,
    kv_latent,
    rope_key,
    latent_gain,
    w_key_up,
    w_value_up,
    query_gain,
    key_gain,
    rope_gain,
    out_gain,
    moe_tokens,
    moe_gain,
    routes,
    route_weights,
    w_gate,
    w_up,
    w_down,
):
    tok_rows = queries.shape[0]
    index = lax.axis_index(EP)
    positions = index * tok_rows + jnp.arange(tok_rows, dtype=jnp.int32)

    def attend(raw_queries):
        keys, own = prepare(
            raw_queries, kv_latent, rope_key, latent_gain, w_key_up, w_value_up, query_gain, key_gain, rope_gain, positions
        )
        keys = lax.all_gather(keys, "ep_0", axis=0, tiled=True)
        shifts = (0, 1, 3, 2)
        pair = jnp.concatenate([own, shifted(own, CORE, 1)], axis=0)
        pieces = [pair] + [shifted(pair, "ep_1", s) for s in shifts[1:]]
        row = lax.axis_index("ep_1")
        core = lax.axis_index(CORE)
        places = [((row - s) & 3) * 2 + (core ^ away) for s in shifts for away in (0, 1)]
        at = jnp.stack([lax.axis_index("ep_0"), row * 2 + core] + places).astype(jnp.int32)
        return flash(at, pieces, keys, lax.axis_size("ep_0"), query_gain.shape[0] ** -0.5)

    moe_out, parts = experts_part(
        moe_tokens, moe_gain, routes, route_weights, w_gate, w_up, w_down, queries, attend
    )
    parts = lax.psum_scatter(parts, YC, scatter_dimension=0, tiled=True)
    attended = finish(parts, out_gain, 1, tok_rows)
    return (attended, moe_out)


def solution(mesh):
    finer = Mesh(mesh.devices.reshape(8, 4, 2, mesh.shape["tp"]), ("ep_0", "ep_1", "ep_2", "tp"))
    placed = (
        P(EP, "tp"),
        P(EP, None),
        P(EP, None),
        P(),
        P(None, "tp"),
        P(None, "tp"),
        P(),
        P(),
        P(),
        P(),
        P(EP, None),
        P(),
        P(EP, None),
        P(EP, None),
        P(EP, None, "tp"),
        P(EP, None, "tp"),
        P(EP, "tp", None),
    )

    return jax.shard_map(
        on_device,
        mesh=finer,
        in_specs=placed,
        out_specs=(P(EP, "tp"), P(EP_TP, None)),
        check_vma=False,
    )
```
